256 devices in a mesh: sp: 16 (over y, x), tp: 16 (over z, core).
Axes of the slice: x: 4, y: 4, z: 8, core: 2. Of those that a mesh axis runs over, the one named last changes fastest.
Arguments:
- residual: bfloat16 [6144, 2048], P(('sp', 'tp')), may hold values from -40 to 40
- queries: bfloat16 [6144, 16, 256], P('sp', 'tp'), may hold values from -8.8 to 8.8
- query_rope: bfloat16 [6144, 16, 64], P('sp', 'tp'), may hold values from -72 to 72
- latent: bfloat16 [6144, 512], P('sp'), may hold values from -320 to 320
- key_rope: bfloat16 [6144, 32], P('sp'), may hold values from -48 to 48
- latent_gain: float32 [512], replicated, may hold values from 0.1 to 1.9
- key_weight: bfloat16 [512, 16, 256], P(None, 'tp'), may hold values from -0.25 to 0.25
- value_weight: bfloat16 [512, 16, 256], P(None, 'tp'), may hold values from -0.25 to 0.25
- out_weight: bfloat16 [16, 256, 2048], P('tp'), may hold values from -0.09375 to 0.09375
- norm_gain: float32 [2048], replicated, may hold values from 0.1 to 1.9
- routes: int32 [6144, 2], P('sp'), may hold values from 0 to 31, as said below
- group_gate: float32 [6144], P(('sp', 'tp')), may hold values from 0.5 to 1
- expert_share: float32 [6144, 2], P(('sp', 'tp')), may hold values from 0.2 to 1
- gate_weight: bfloat16 [32, 2048, 4096], P('sp', None, 'tp'), may hold values from -0.125 to 0.125
- up_weight: bfloat16 [32, 2048, 4096], P('sp', None, 'tp'), may hold values from -0.125 to 0.125
- down_weight: bfloat16 [32, 4096, 2048], P('sp', 'tp'), may hold values from -0.1875 to 0.1875
Outputs:
- layer_out: bfloat16 [6144, 2048], P(('sp', 'tp'))
The draws below stay inside these ranges and needn't reach their ends.
Inputs may be any that keep to these rules, and one draw needn't show every extreme that they name: `routes`: each token names two different experts of one group; expert e belongs to group e // 8. In each aligned block of 24 tokens no expert is named more than 2 times, and one expert, the same in every block, is named exactly 2 times in every block.
All inputs are finite; a program needn't handle non-finite values.
Results may differ from the reference program's by a relative error of at most 0.025.
Values may be sent and summed in bfloat16 or wider, within the bound.
No kernel may reach another device: no remote copies, remote signals or barrier semaphores. Data moves between devices by JAX's collectives and lax.ppermute only.
A program may use at most 64 MiB of HBM per device.

```python
import math
import jax
import jax.numpy as jnp
from jax import lax

D = 2048
PAIRS = 16
DK_A = 64
DV_A = 64
DK_B = 192
DV_B = 192
DR = 32
LATENT = 512
FF = 4096
GROUPS = 4
TOPK = 2
SEQ = 6144
PAIR_DEV = 1
ROWS = 24
FF_DEV = 256
EXPERTS = 32
CAP = 2
N_TP = 16


def rough_field(key, salt_value, columns):
    values = jnp.clip(jax.random.normal(jax.random.fold_in(key, salt_value), (SEQ, columns), jnp.float32), -4.0, 4.0)
    return values


def draw_residual(key, part):
    return (0.25 * rough_field(key, 40, D)).astype(jnp.bfloat16)


def draw_latent(key, part):
    return rough_field(key, 50, LATENT).astype(jnp.bfloat16)


def draw_queries(key, part):
    own_key = jax.random.fold_in(key, 23)
    array_shape = (SEQ, PAIRS, DK_A + DK_B)
    return jnp.clip(2.2 * jax.random.normal(own_key, array_shape, jnp.float32), -8.75, 8.75).astype(jnp.bfloat16)


def draw_query_rope(key, part):
    own_key = jax.random.fold_in(key, 21)
    array_shape = (SEQ, PAIRS, 2 * DR)
    return jnp.clip(2.2 * jax.random.normal(own_key, array_shape, jnp.float32), -8.75, 8.75).astype(jnp.bfloat16)


def draw_key_rope(key, part):
    own_key = jax.random.fold_in(key, 22)
    base_values = jnp.clip(jax.random.normal(own_key, (SEQ, DR), jnp.float32), -4.0, 4.0)
    return base_values.astype(jnp.bfloat16)


def draw_routes(key, part):
    blocks = SEQ // ROWS
    within = EXPERTS // GROUPS
    pair_total = EXPERTS // 2
    hot_rows = 0
    while hot_rows + (ROWS - hot_rows + pair_total - 1) // pair_total != CAP:
        hot_rows += 1
    key_list = jax.random.split(jax.random.fold_in(key, 31), 5)
    favored = jax.random.randint(key_list[0], (), 0, EXPERTS, dtype=jnp.int32)
    favored_group = favored // within
    favored_place = favored % within
    member = jnp.arange(within, dtype=jnp.int32)
    ranking = jax.random.randint(key_list[1], (blocks, GROUPS, within), 0, 1 << 20, dtype=jnp.int32) * within + member
    place_order = jnp.argsort(ranking, axis=2).astype(jnp.int32)
    leading = place_order[:, :, :1]
    swapped = jnp.where(place_order == favored_place, leading, place_order)
    swapped = jnp.where(member[None, None, :] == 0, favored_place, swapped)
    is_favored = (jnp.arange(GROUPS, dtype=jnp.int32) == favored_group)[None, :, None]
    place_order = jnp.where(is_favored, swapped, place_order)
    expert_table = place_order + (jnp.arange(GROUPS, dtype=jnp.int32) * within)[None, :, None]
    pair_table = expert_table.reshape(blocks, pair_total, 2)
    pair_ids = jnp.arange(pair_total, dtype=jnp.int32)
    pair_rank = jax.random.randint(key_list[2], (blocks, pair_total), 0, 1 << 20, dtype=jnp.int32) * pair_total + pair_ids
    pair_rank = jnp.where(pair_ids[None, :] == favored_group * (within // 2), -1, pair_rank)
    pair_order = jnp.argsort(pair_rank, axis=1)
    pair_table = jnp.take_along_axis(pair_table, pair_order[:, :, None], axis=1)
    row_ids = jnp.arange(ROWS, dtype=jnp.int32)
    cycled = jnp.take(pair_table, (row_ids - hot_rows) % pair_total, axis=1)
    favored_row = jnp.take(expert_table, favored_group, axis=1)
    partner = jnp.take(favored_row, 1 + row_ids % (within - 1), axis=1)
    hot_pair = jnp.stack([jnp.broadcast_to(favored, partner.shape), partner], axis=2)
    chosen = jnp.where((row_ids < hot_rows)[None, :, None], hot_pair, cycled)
    flip_bits = jax.random.randint(key_list[3], (blocks, ROWS, 1), 0, 2, dtype=jnp.int32)
    chosen = jnp.where(flip_bits == 1, chosen[:, :, ::-1], chosen)
    shuffle = jnp.argsort(jax.random.randint(key_list[4], (blocks, ROWS), 0, 1 << 20, dtype=jnp.int32) * ROWS + row_ids[None, :], axis=1)
    chosen = jnp.take_along_axis(chosen, shuffle[:, :, None], axis=1)
    return chosen.reshape(SEQ, 2).astype(jnp.int32)


def block_levels(rng, shape, pieces, smallest, top_value):
    def one(axis_at, parts):
        steps = jax.random.uniform(jax.random.fold_in(jax.random.fold_in(rng, 6), axis_at), (parts,), jnp.float32, smallest / len(pieces), top_value / len(pieces))
        return jnp.repeat(jnp.exp(steps), shape[axis_at] // parts).reshape((-1,) + (1,) * (len(shape) - axis_at - 1))

    level = one(*pieces[0])
    for cut in pieces[1:]:
        level = level * one(*cut)
    return level


def scatter_about(key, shape, deviation, limit, cuts=(), kind=jnp.bfloat16):
    array = jax.random.normal(key, shape, jnp.float32) * deviation
    if len(cuts) > 0:
        array = block_levels(key, shape, cuts, -0.22, 0.18) * array
    return jnp.clip(array, min=-limit, max=limit).astype(kind)


def setup_inputs(seed: int = 0) -> dict:
    splits = jax.random.split(jax.random.key(seed), 17)
    residual = draw_residual(jax.random.fold_in(splits[16], 71), 0)
    queries = draw_queries(jax.random.fold_in(splits[16], 71), 0)
    query_rope = draw_query_rope(jax.random.fold_in(splits[16], 71), 0)
    latent = draw_latent(jax.random.fold_in(splits[16], 71), 0)
    key_rope = draw_key_rope(jax.random.fold_in(splits[16], 71), 0)
    latent_gain = jnp.clip(1.0 + 0.18 * jax.random.normal(splits[5], (LATENT,), jnp.float32), 0.1, 1.9)
    key_weight = scatter_about(splits[6], (LATENT, PAIRS, DK_A + DK_B), LATENT ** -0.5, 0.25, ((1, 16),))
    value_weight = scatter_about(splits[7], (LATENT, PAIRS, DV_A + DV_B), LATENT ** -0.5, 0.25, ((1, 16),))
    out_weight = scatter_about(splits[8], (PAIRS, DV_A + DV_B, D), (PAIRS * (DV_A + DV_B)) ** -0.5, 0.09375, ((0, 16),))
    norm_gain = jnp.clip(1.0 + 0.18 * jax.random.normal(splits[9], (D,), jnp.float32), 0.1, 1.9)
    routes = draw_routes(jax.random.fold_in(splits[16], 71), 0)
    group_gate = jnp.clip(jnp.exp(math.log(1.0) - 0.6931472 * jax.random.uniform(splits[11], (SEQ,), jnp.float32) ** block_levels(splits[11], (SEQ,), ((0, 256),), -0.2, 0.2)), 0.5, 1.0)
    expert_share = jnp.clip(jnp.exp(math.log(1.0) - 1.609438 * jax.random.uniform(splits[12], (SEQ, TOPK), jnp.float32) ** block_levels(splits[12], (SEQ, TOPK), ((0, 256),), -0.2, 0.2)), 0.2, 1.0)
    gate_weight = scatter_about(splits[13], (EXPERTS, D, FF), D ** -0.5, 0.125, ((0, 16), (2, 16)))
    up_weight = scatter_about(splits[14], (EXPERTS, D, FF), D ** -0.5, 0.125, ((0, 16), (2, 16)))
    down_weight = scatter_about(splits[15], (EXPERTS, FF, D), (FF // 4) ** -0.5, 0.1875, ((0, 16), (1, 16)))
    return {"residual": residual, "queries": queries, "query_rope": query_rope, "latent": latent, "key_rope": key_rope, "latent_gain": latent_gain, "key_weight": key_weight, "value_weight": value_weight, "out_weight": out_weight, "norm_gain": norm_gain, "routes": routes, "group_gate": group_gate, "expert_share": expert_share, "gate_weight": gate_weight, "up_weight": up_weight, "down_weight": down_weight}


rope_base = 10000.0
epsilon = 1e-06

def angle_tables(places, rope_width):
    frequencies = rope_base ** (-jnp.arange(0, rope_width, 2, dtype=jnp.float32) / rope_width)
    angles = places[:, None] * frequencies[None, :]
    return (jnp.cos(angles), jnp.sin(angles))

def rope_turn(values, cosine, sine_table):
    half_size = values.shape[-1] // 2
    first_half = values[..., :half_size]
    second = values[..., half_size:]
    return jnp.concatenate([first_half * cosine - second * sine_table, second * cosine + first_half * sine_table], axis=-1)

def rms_scale(values, gain_vector):
    values = values.astype(jnp.float32)
    inverse = lax.rsqrt(lax.optimization_barrier(jnp.mean(values * values, axis=-1, keepdims=True)) + epsilon)
    return values * inverse * gain_vector.astype(jnp.float32)

def group_attend(query_nope, query_turned, key_nope, rotated_key, value_part, visible, scale):
    scores = jnp.einsum('qhd,khd->hqk', query_nope.astype(jnp.float32), key_nope.astype(jnp.float32))
    scores = scores + jnp.einsum('qhd,kd->hqk', query_turned.astype(jnp.float32), rotated_key.astype(jnp.float32))
    scores = scores * scale
    masked = jnp.where(visible[None], scores, -jnp.inf)
    row_top = lax.optimization_barrier(jnp.max(masked, axis=2, keepdims=True))
    weights = jnp.exp(masked - row_top)
    weight_sum = lax.optimization_barrier(jnp.sum(weights, axis=2))
    rounded = lax.optimization_barrier(weights.astype(jnp.bfloat16)).astype(jnp.float32)
    mixed_rows = jnp.einsum('hqk,khd->qhd', rounded, value_part.astype(jnp.float32))
    return (mixed_rows / jnp.transpose(weight_sum)[:, :, None]).astype(jnp.bfloat16)

def reference(residual, queries, query_rope, latent, key_rope, latent_gain, key_weight, value_weight, out_weight, norm_gain, routes, group_gate, expert_share, gate_weight, up_weight, down_weight):
    places = jnp.arange(SEQ, dtype=jnp.int32).astype(jnp.float32)
    cosine, sine_table = angle_tables(places, DR)
    compressed = rms_scale(latent, latent_gain).astype(jnp.bfloat16)
    rotated_key = rope_turn(key_rope.astype(jnp.float32), cosine, sine_table).astype(jnp.bfloat16)
    turned = rope_turn(query_rope.astype(jnp.float32).reshape(SEQ, PAIRS, 2, DR), cosine[:, None, None, :], sine_table[:, None, None, :]).astype(jnp.bfloat16)
    key_rows = jnp.dot(compressed, key_weight.reshape(LATENT, -1), preferred_element_type=jnp.float32).astype(jnp.bfloat16).reshape(SEQ, PAIRS, DK_A + DK_B)
    value_rows = jnp.dot(compressed, value_weight.reshape(LATENT, -1), preferred_element_type=jnp.float32).astype(jnp.bfloat16).reshape(SEQ, PAIRS, DV_A + DV_B)
    scale_one = (DK_A + DR) ** (-0.5)
    scale_two = (DK_B + DR) ** (-0.5)
    block_size = 256

    def attend_block(block_index):
        block_start = block_index * block_size
        query_block = lax.dynamic_slice_in_dim(queries, block_start, block_size, 0)
        turned_block = lax.dynamic_slice_in_dim(turned, block_start, block_size, 0)
        query_places = (block_start + jnp.arange(block_size, dtype=jnp.int32)).astype(jnp.float32)
        visible = query_places[:, None] >= places[None, :]
        part_one = group_attend(query_block[:, :, :DK_A], turned_block[:, :, 0], key_rows[:, :, :DK_A], rotated_key, value_rows[:, :, :DV_A], visible, scale_one)
        part_two = group_attend(query_block[:, :, DK_A:], turned_block[:, :, 1], key_rows[:, :, DK_A:], rotated_key, value_rows[:, :, DV_A:], visible, scale_two)
        return jnp.concatenate([part_one, part_two], axis=2)
    attention = lax.map(attend_block, jnp.arange(SEQ // block_size, dtype=jnp.int32)).reshape(SEQ, PAIRS * (DV_A + DV_B))
    out_flat = out_weight.reshape(PAIRS * (DV_A + DV_B), D)
    run_width = PAIR_DEV * (DV_A + DV_B)

    def add_run(running, run_index):
        columns = lax.dynamic_slice_in_dim(attention, run_index * run_width, run_width, 1)
        weight_rows = lax.dynamic_slice_in_dim(out_flat, run_index * run_width, run_width, 0)
        partial_sum = jnp.dot(columns, weight_rows, preferred_element_type=jnp.float32)
        return (running + lax.optimization_barrier(partial_sum.astype(jnp.bfloat16)).astype(jnp.float32), None)
    head_total, unused = lax.scan(add_run, jnp.zeros((SEQ, D), jnp.float32), jnp.arange(N_TP, dtype=jnp.int32))
    mixed_rows = residual.astype(jnp.float32) + head_total
    normed = rms_scale(mixed_rows, norm_gain).astype(jnp.bfloat16)
    blocks = SEQ // ROWS
    flat_routes = routes.reshape(blocks, ROWS * TOPK)
    onehot = (flat_routes[:, :, None] == jnp.arange(EXPERTS, dtype=jnp.int32)[None, None, :]).astype(jnp.int32)
    rank_within = lax.optimization_barrier(jnp.sum((jnp.cumsum(onehot, axis=1) - onehot) * onehot, axis=2))
    slot_columns = (jnp.arange(blocks, dtype=jnp.int32)[:, None] * CAP + rank_within).reshape(-1).astype(jnp.int32)
    expert_flat = flat_routes.reshape(-1).astype(jnp.int32)
    token_flat = jnp.repeat(jnp.arange(SEQ, dtype=jnp.int32), TOPK)
    token_of = jnp.full((EXPERTS, blocks * CAP), SEQ, dtype=jnp.int32).at[expert_flat, slot_columns].set(token_flat)
    padded = jnp.concatenate([normed, jnp.zeros((1, D), jnp.bfloat16)], axis=0)
    expert_rows = padded[token_of]

    def expert_apply(inputs):
        rows_in, gate_part, up_part, down_part = inputs
        gate_out = jnp.dot(rows_in, gate_part, preferred_element_type=jnp.float32)
        up_out = jnp.dot(rows_in, up_part, preferred_element_type=jnp.float32)
        hidden = (jax.nn.silu(gate_out) * up_out).astype(jnp.bfloat16)
        hidden_runs = hidden.reshape(hidden.shape[0], N_TP, FF_DEV).astype(jnp.float32)
        down_runs = down_part.reshape(N_TP, FF_DEV, D).astype(jnp.float32)
        partial_sum = jnp.einsum('snf,nfd->snd', hidden_runs, down_runs)
        rounded = lax.optimization_barrier(partial_sum.astype(jnp.bfloat16)).astype(jnp.float32)
        return lax.optimization_barrier(jnp.sum(rounded, axis=1)).astype(jnp.bfloat16)
    outputs = lax.map(expert_apply, (expert_rows, gate_weight, up_weight, down_weight))
    picked = outputs[expert_flat, slot_columns].astype(jnp.float32).reshape(SEQ, TOPK, D)
    share_values = expert_share.astype(jnp.float32)
    route_weight = group_gate.astype(jnp.float32)[:, None] * share_values / lax.optimization_barrier(jnp.sum(share_values, axis=1, keepdims=True))
    expert_mix = lax.optimization_barrier(jnp.sum(route_weight[:, :, None] * picked, axis=1))
    return (mixed_rows + expert_mix).astype(jnp.bfloat16)
```

```python
import functools

import jax
import jax.numpy as jnp
from jax import lax
from jax.experimental import pallas as pl
from jax.experimental.pallas import tpu as pltpu
from jax.sharding import Mesh
from jax.sharding import PartitionSpec as P

AXES = ("y", "x", "z", "c")
SP = ("y", "x")
NY, NX, NZ, NC = 4, 4, 8, 2
DK_A = 64
DV_A = 64
ROPE = 32
CAP = 2
LOG2E = 1.4426950408889634

rope_base = 10000.0
epsilon = 1e-06
floor_score = -1e30


def flat(y, x, z, c):
    return ((y * NX + x) * NZ + z) * NC + c


def moves(target):
    pairs = []
    for y in range(NY):
        for x in range(NX):
            for z in range(NZ):
                for c in range(NC):
                    pairs.append((flat(y, x, z, c), flat(*target(y, x, z, c))))
    return pairs


def first_axis(step):
    return moves(
        lambda y, x, z, c: ((y + step) % NY, x, z, c) if c == 0 else (y, (x + step) % NX, z, c)
    )


def second_axis(step):
    return moves(
        lambda y, x, z, c: (y, (x + step) % NX, z, c) if c == 0 else ((y + step) % NY, x, z, c)
    )


def ring(sign):
    return moves(lambda y, x, z, c: (y, x, (z + (sign if c == 0 else -sign)) % NZ, c))


PARTNER = moves(lambda y, x, z, c: (y, x, z, 1 - c))


def send(value, pairs):
    return lax.ppermute(value, AXES, pairs)


def swap(value):
    return lax.ppermute(value, AXES, PARTNER)


def angle_tables(places, rope_width):
    frequencies = rope_base ** (-jnp.arange(0, rope_width, 2, dtype=jnp.float32) / rope_width)
    angles = places[:, None] * frequencies[None, :]
    return (jnp.cos(angles), jnp.sin(angles))


def rope_turn(values, cosine, sine_table):
    half_size = values.shape[-1] // 2
    first_half = values[..., :half_size]
    second = values[..., half_size:]
    return jnp.concatenate(
        [first_half * cosine - second * sine_table, second * cosine + first_half * sine_table],
        axis=-1,
    )


def rms_scale(values, gain_vector):
    values = values.astype(jnp.float32)
    inverse = lax.rsqrt(jnp.mean(values * values, axis=-1, keepdims=True) + epsilon)
    return values * inverse * gain_vector


def attend_kernel(counts, first, last, scale_one, scale_two, *refs):
    n = len(counts)
    info_ref, qa_ref, qb_ref, wk_ref, wv_ref = refs[:5]
    piece_refs = refs[5 : 5 + n]
    if first:
        rest = refs[5 + n :]
    else:
        stat_in, acc_in = refs[5 + n : 7 + n]
        rest = refs[7 + n :]
    if last:
        out_ref, stat_ref, acc_ref = rest
    else:
        stat_ref, acc_ref = rest
    contract = (((1,), (1,)), ((), ()))
    if first:
        rows = lax.broadcasted_iota(jnp.int32, stat_ref.shape, 0)
        stat_ref[...] = jnp.where(rows < 2, floor_score, 0.0)
        acc_ref[...] = jnp.zeros(acc_ref.shape, jnp.float32)
    else:
        stat_ref[...] = stat_in[...]
        acc_ref[...] = acc_in[...]
    own_start = info_ref[0]

    def head(keys, q_ref, values, scale, row, lo, hi, visible):
        scores = lax.dot_general(
            keys, q_ref[...], contract, preferred_element_type=jnp.float32
        ) * (scale * LOG2E)
        if visible is not None:
            scores = jnp.where(visible, scores, floor_score)
        old_top = stat_ref[row : row + 1, :]
        new_top = jnp.maximum(old_top, jnp.max(scores, axis=0, keepdims=True))
        weights = jnp.exp2(scores - new_top)
        factor = jnp.exp2(old_top - new_top)
        stat_ref[row : row + 1, :] = new_top
        stat_ref[row + 2 : row + 3, :] = stat_ref[row + 2 : row + 3, :] * factor + jnp.sum(
            weights, axis=0, keepdims=True
        )
        acc_ref[lo:hi, :] = acc_ref[lo:hi, :] * factor + jnp.dot(
            values, weights.astype(jnp.bfloat16), preferred_element_type=jnp.float32
        )

    offset = 1
    for piece_ref, count in zip(piece_refs, counts):

        def one(i, carry, piece_ref=piece_ref, offset=offset):
            start = info_ref[offset + i]

            def work():
                piece = piece_ref[i]
                keys = jnp.dot(piece, wk_ref[...], preferred_element_type=jnp.float32).astype(
                    jnp.bfloat16
                )
                values = lax.dot_general(
                    wv_ref[...], piece[:, :512], contract, preferred_element_type=jnp.float32
                ).astype(jnp.bfloat16)
                visible = None
                if first:
                    shape = (piece.shape[0], qa_ref.shape[0])
                    key_at = start + lax.broadcasted_iota(jnp.int32, shape, 0)
                    query_at = own_start + lax.broadcasted_iota(jnp.int32, shape, 1)
                    visible = query_at >= key_at
                head(keys[:, :128], qa_ref, values[:DV_A], scale_one, 0, 0, DV_A, visible)
                head(keys[:, 128:], qb_ref, values[DV_A:], scale_two, 1, DV_A, 256, visible)

            if first:
                work()
            else:
                pl.when(start < own_start)(work)
            return carry

        lax.fori_loop(0, count, one, 0)
        offset += count
    if last:
        out_ref[:DV_A, :] = (acc_ref[:DV_A, :] / stat_ref[2:3, :]).astype(jnp.bfloat16)
        out_ref[DV_A:, :] = (acc_ref[DV_A:, :] / stat_ref[3:4, :]).astype(jnp.bfloat16)


def attend(info, qa, qb, wk, wv, pieces, state, last, scales):
    counts = tuple(p.shape[0] for p in pieces)
    first = state is None
    tokens = qa.shape[0]
    vmem = pl.BlockSpec(memory_space=pltpu.VMEM)
    in_specs = [pl.BlockSpec(memory_space=pltpu.SMEM)] + [vmem] * (4 + len(pieces))
    args = [info, qa, qb, wk, wv, *pieces]
    if not first:
        args += list(state)
        in_specs += [vmem, vmem]
    stat = jax.ShapeDtypeStruct((8, tokens), jnp.float32)
    acc = jax.ShapeDtypeStruct((256, tokens), jnp.float32)
    if last:
        out_shape = jax.ShapeDtypeStruct((256, tokens), jnp.bfloat16)
        out_specs = vmem
        scratch = [pltpu.VMEM(stat.shape, stat.dtype), pltpu.VMEM(acc.shape, acc.dtype)]
    else:
        out_shape = (stat, acc)
        out_specs = (vmem, vmem)
        scratch = []
    total = sum(counts) * pieces[0].shape[1]
    return pl.pallas_call(
        functools.partial(attend_kernel, counts, first, last, *scales),
        in_specs=in_specs,
        out_specs=out_specs,
        out_shape=out_shape,
        scratch_shapes=scratch,
        cost_estimate=pl.CostEstimate(
            flops=2 * total * (640 * 384 + 512 * 256 + tokens * 640),
            bytes_accessed=total * 1280,
            transcendentals=2 * total * tokens,
        ),
        compiler_params=pltpu.CompilerParams(vmem_limit_bytes=40 * 1024 * 1024),
        name="attend",
    )(*args)


def slot_table(route_block, experts_all, capacity):
    flat_routes = route_block.reshape(-1)
    onehot = (flat_routes[:, None] == jnp.arange(experts_all, dtype=jnp.int32)[None, :]).astype(
        jnp.int32
    )
    rank_within = jnp.sum((jnp.cumsum(onehot, axis=0) - onehot) * onehot, axis=1)
    return flat_routes * capacity + rank_within


def own_half(value, core, dim):
    half = value.shape[dim] // 2
    low = lax.slice_in_dim(value, 0, half, axis=dim)
    high = lax.slice_in_dim(value, half, 2 * half, axis=dim)
    first = core == 0
    return jnp.where(first, low, high), jnp.where(first, high, low)


def local(
    residual,
    queries,
    query_rope,
    latent,
    key_rope,
    latent_gain,
    key_weight,
    value_weight,
    out_weight,
    norm_gain,
    routes,
    group_gate,
    expert_share,
    gate_weight,
    up_weight,
    down_weight,
):
    tokens = queries.shape[0]
    half_rows = tokens // 2
    row_count = residual.shape[0]
    width = residual.shape[1]
    iy, ix, iz, core = (lax.axis_index(a) for a in AXES)
    index = iy * NX + ix
    first_place = index * tokens
    places = (first_place + jnp.arange(tokens, dtype=jnp.int32)).astype(jnp.float32)
    cosine, sine_table = angle_tables(places, ROPE)
    rotated_key = rope_turn(key_rope.astype(jnp.float32), cosine, sine_table).astype(jnp.bfloat16)
    compressed = rms_scale(latent, latent_gain).astype(jnp.bfloat16)
    rows = jnp.concatenate(
        [compressed, rotated_key, jnp.zeros((tokens, 96), jnp.bfloat16)], axis=1
    ).reshape(2, half_rows, 640)
    own_piece = jnp.where(core == 0, rows[0], rows[1])

    out_flat = out_weight[0]
    out_keep, out_give = own_half(out_flat, core, 1)
    out_got = swap(out_give)
    down_other = swap(down_weight)

    turned = rope_turn(
        query_rope[:, 0].astype(jnp.float32).reshape(tokens, 2, ROPE),
        cosine[:, None, :],
        sine_table[:, None, :],
    ).astype(jnp.bfloat16)
    flat_queries = queries[:, 0]
    pad = jnp.zeros((tokens, 32), jnp.bfloat16)
    qa = jnp.concatenate([flat_queries[:, :DK_A], turned[:, 0], pad], axis=1)
    qb = jnp.concatenate([flat_queries[:, DK_A:], turned[:, 1], pad], axis=1)
    eye = jnp.eye(128, ROPE, dtype=jnp.bfloat16)
    keys_flat = key_weight[:, 0]
    top = jnp.zeros((512, ROPE), jnp.bfloat16)
    wk = jnp.concatenate(
        [
            jnp.concatenate([keys_flat[:, :DK_A], jnp.zeros((128, DK_A), jnp.bfloat16)], axis=0),
            jnp.concatenate([top, eye], axis=0),
            jnp.zeros((640, 32), jnp.bfloat16),
            jnp.concatenate([keys_flat[:, DK_A:], jnp.zeros((128, 192), jnp.bfloat16)], axis=0),
            jnp.concatenate([top, eye], axis=0),
            jnp.zeros((640, 32), jnp.bfloat16),
        ],
        axis=1,
    )
    wv = value_weight[:, 0].T
    scales = ((DK_A + ROPE) ** (-0.5), (queries.shape[2] - DK_A + ROPE) ** (-0.5))

    def starts(turn, along, across):
        out = []
        for a in along:
            ya = jnp.where(turn == 0, iy + a, iy + across) % NY
            xa = jnp.where(turn == 0, ix + across, ix + a) % NX
            out.append((ya * NX + xa) * tokens + turn * half_rows)
        return out

    other = 1 - core
    call = functools.partial(attend, qa=qa, qb=qb, wk=wk, wv=wv, scales=scales)

    def info(entries):
        return jnp.stack([first_place] + entries).astype(jnp.int32)

    behind = send(own_piece, first_axis(1))
    ahead = send(own_piece, first_axis(-1))
    across = send(own_piece, first_axis(2))
    state = attend(
        info([first_place, first_place + half_rows]),
        qa, qb, wk, wv, [rows], None, False, scales,
    )
    line = jnp.stack([own_piece, behind, ahead, across])
    order = (0, -1, 1, 2)
    line_behind = send(line, second_axis(1))
    line_ahead = send(line, second_axis(-1))
    line_swap = swap(line[1:])
    state = attend(
        info(starts(core, order, 0) + starts(other, order[1:], 0)),
        qa, qb, wk, wv, [line, line_swap], state, False, scales,
    )
    far_low = send(line_behind[:2], second_axis(1))
    far_high = send(line_ahead[2:], second_axis(-1))
    behind_swap = swap(line_behind)
    ahead_swap = swap(line_ahead)
    state = attend(
        info(
            starts(core, order, -1)
            + starts(core, order, 1)
            + starts(other, order, -1)
            + starts(other, order, 1)
        ),
        qa, qb, wk, wv, [line_behind, line_ahead, behind_swap, ahead_swap], state, False, scales,
    )
    low_swap = swap(far_low)
    high_swap = swap(far_high)
    attention = attend(
        info(
            starts(core, order[:2], 2)
            + starts(core, order[2:], 2)
            + starts(other, order[:2], 2)
            + starts(other, order[2:], 2)
        ),
        qa, qb, wk, wv, [far_low, far_high, low_swap, high_swap], state, True, scales,
    )

    both = jnp.concatenate([attention, swap(attention)], axis=0)
    out_both = jnp.concatenate([out_keep, out_got], axis=0)
    partial_rows = lax.dot_general(
        both, out_both, (((0,), (0,)), ((), ())), preferred_element_type=jnp.float32
    ).astype(jnp.bfloat16)
    arrived = lax.all_to_all(
        partial_rows.reshape(NZ, 2 * row_count, width // 2), "z", 0, 0, tiled=True
    )
    summed = arrived.astype(jnp.float32).sum(axis=0)
    keep, give = own_half(summed, core, 0)
    got = swap(give)
    head_total = jnp.where(
        core == 0, jnp.concatenate([keep, got], axis=1), jnp.concatenate([got, keep], axis=1)
    )
    mixed_rows = residual.astype(jnp.float32) + head_total
    normed = rms_scale(mixed_rows, norm_gain).astype(jnp.bfloat16)

    experts_dev = gate_weight.shape[0]
    sp_count = NY * NX
    experts_all = experts_dev * sp_count
    top_count = routes.shape[1]
    slot_count = experts_all * CAP
    own_routes = lax.dynamic_slice_in_dim(routes, (iz * NC + core) * row_count, row_count, 0)
    own_slots = slot_table(own_routes, experts_all, CAP)
    pick_matrix = (jnp.arange(slot_count, dtype=jnp.int32)[:, None] == own_slots[None, :]).astype(
        jnp.bfloat16
    )
    pick_matrix = pick_matrix.reshape(slot_count, row_count, top_count).sum(axis=2)
    outgoing = jnp.dot(pick_matrix, normed, preferred_element_type=jnp.float32).astype(jnp.bfloat16)
    arrived_rows = lax.all_to_all(
        outgoing.reshape(sp_count, experts_dev * CAP, width), SP, 0, 0, tiled=True
    ).reshape(slot_count, width)
    slot = jnp.arange(slot_count, dtype=jnp.int32)
    per = sp_count * CAP
    source = (slot % per) // CAP * (experts_dev * CAP) + slot // per * CAP + slot % CAP
    shuffle = (source[:, None] == slot[None, :]).astype(jnp.bfloat16)
    own = jnp.dot(shuffle, arrived_rows, preferred_element_type=jnp.float32).astype(jnp.bfloat16)

    down_both = jnp.concatenate([down_weight, down_other], axis=1)

    def hidden_of(blocks):
        out = []
        for e in range(experts_dev):
            stacked = jnp.concatenate([b[e * per : (e + 1) * per] for b in blocks], axis=0)
            gate_out = jnp.dot(stacked, gate_weight[e], preferred_element_type=jnp.float32)
            up_out = jnp.dot(stacked, up_weight[e], preferred_element_type=jnp.float32)
            out.append((jax.nn.silu(gate_out) * up_out).astype(jnp.bfloat16))
        return jnp.stack(out)

    def outputs_of(mine, theirs):
        count = len(mine)
        hidden = hidden_of(mine + theirs)
        keep_hidden = hidden[:, : count * per]
        got_hidden = swap(hidden[:, count * per :])
        result = [
            jnp.dot(
                jnp.concatenate([keep_hidden[e], got_hidden[e]], axis=1),
                down_both[e],
                preferred_element_type=jnp.float32,
            )
            for e in range(experts_dev)
        ]
        return [
            jnp.concatenate([r[i * per : (i + 1) * per] for r in result], axis=0)
            for i in range(count)
        ]

    onward = ring(1)
    back = ring(-1)
    par = swap(own)
    m1 = send(own, onward)
    p1 = send(par, onward)
    m2 = send(m1, onward)
    p2 = send(p1, onward)
    m3 = send(m2, onward)
    p3 = send(p2, onward)
    m4 = send(m3, onward)
    (o_own,) = outputs_of([own], [par])
    o_m1, o_p1 = outputs_of([m1, p1], [swap(m1), swap(p1)])
    o_m2, o_p2 = outputs_of([m2, p2], [swap(m2), swap(p2)])
    o_m3, o_p3 = outputs_of([m3, p3], [swap(m3), swap(p3)])
    (o_m4,) = outputs_of([m4], [swap(m4)])

    def hop(value, addend):
        return (send(value, back).astype(jnp.float32) + addend).astype(jnp.bfloat16)

    chain_p = hop(o_p3.astype(jnp.bfloat16), o_p2)
    chain_m = hop(o_m4.astype(jnp.bfloat16), o_m3)
    chain_p = hop(chain_p, o_p1)
    chain_m = hop(chain_m, o_m2)
    chain_p = swap(send(chain_p, back))
    chain_m = hop(chain_m, o_m1)
    chain_m = send(chain_m, back)
    total = (o_own + chain_m.astype(jnp.float32) + chain_p.astype(jnp.float32)).astype(jnp.bfloat16)

    unshuffled = lax.dot_general(
        shuffle, total, (((0,), (0,)), ((), ())), preferred_element_type=jnp.float32
    ).astype(jnp.bfloat16)
    returned = lax.all_to_all(
        unshuffled.reshape(sp_count, experts_dev * CAP, width), SP, 0, 0, tiled=True
    ).reshape(slot_count, width)
    selectors = (own_slots[:, None] == slot[None, :]).astype(jnp.bfloat16)
    picked = jnp.dot(selectors, returned, preferred_element_type=jnp.float32).reshape(
        row_count, top_count, -1
    )
    route_weight = group_gate[:, None] * expert_share / jnp.sum(expert_share, axis=1, keepdims=True)
    expert_mix = jnp.sum(route_weight[:, :, None] * picked, axis=1)
    return (mixed_rows + expert_mix).astype(jnp.bfloat16)


def solution(mesh):
    finer = Mesh(mesh.devices.reshape(NY, NX, NZ, NC), AXES)
    tp = ("z", "c")
    placed = (
        P(AXES, None),
        P(SP, tp, None),
        P(SP, tp, None),
        P(SP, None),
        P(SP, None),
        P(),
        P(None, tp, None),
        P(None, tp, None),
        P(tp, None, None),
        P(),
        P(SP, None),
        P(AXES),
        P(AXES, None),
        P(SP, None, tp),
        P(SP, None, tp),
        P(SP, tp, None),
    )
    return jax.shard_map(
        local, mesh=finer, in_specs=placed, out_specs=P(AXES, None), check_vma=False
    )
```

```python
import functools

import jax
import jax.numpy as jnp
from jax import lax
from jax.experimental import pallas as pl
from jax.experimental.pallas import tpu as pltpu
from jax.sharding import Mesh
from jax.sharding import PartitionSpec as P


AXES = ("y", "x", "z", "c")
SP = ("y", "x")
NY, NX, NZ, NC = 4, 4, 8, 2
DK_A = 64
DV_A = 64
ROPE = 32
CAP = 2
LOG2E = 1.4426950408889634

rope_base = 10000.0
epsilon = 1e-06
floor_score = -1e30


def flat(y, x, z, c):
    return ((y * NX + x) * NZ + z) * NC + c


def moves(target):
    pairs = []
    for y in range(NY):
        for x in range(NX):
            for z in range(NZ):
                for c in range(NC):
                    pairs.append((flat(y, x, z, c), flat(*target(y, x, z, c))))
    return pairs


def first_axis(step):
    return moves(
        lambda y, x, z, c: ((y + step) % NY, x, z, c) if c == 0 else (y, (x + step) % NX, z, c)
    )


def second_axis(step):
    return moves(
        lambda y, x, z, c: (y, (x + step) % NX, z, c) if c == 0 else ((y + step) % NY, x, z, c)
    )


def ring(sign):
    return moves(lambda y, x, z, c: (y, x, (z + (sign if c == 0 else -sign)) % NZ, c))


PARTNER = moves(lambda y, x, z, c: (y, x, z, 1 - c))


def send(value, pairs):
    return lax.ppermute(value, AXES, pairs)


def swap(value):
    return lax.ppermute(value, AXES, PARTNER)


def rms_scale(values, gain_vector):
    values = values.astype(jnp.float32)
    inverse = lax.rsqrt(jnp.mean(values * values, axis=-1, keepdims=True) + epsilon)
    return values * inverse * gain_vector


def turn(values, cos_ref, sin_ref):
    cosine, sine = cos_ref[...], sin_ref[...]
    values = values.astype(jnp.float32)
    out = []
    for lo in range(0, values.shape[0], ROPE):
        u = values[lo : lo + ROPE // 2]
        w = values[lo + ROPE // 2 : lo + ROPE]
        out += [u * cosine - w * sine, w * cosine + u * sine]
    return jnp.concatenate(out, axis=0).astype(jnp.bfloat16)


ROWS_OF_BOTH = (((0,), (0,)), ((), ()))


def latent_kernel(core_ref, latent_ref, gain_ref, rope_ref, cos_ref, sin_ref, rows_ref, own_ref):
    half = latent_ref.shape[0] // 2
    compressed = rms_scale(latent_ref[...], gain_ref[...]).astype(jnp.bfloat16)
    turned = turn(rope_ref[...], cos_ref, sin_ref)
    row = lax.broadcasted_iota(jnp.int32, (ROPE, 128), 0)
    col = lax.broadcasted_iota(jnp.int32, (ROPE, 128), 1)
    wide = lax.dot_general(
        turned, (row == col).astype(jnp.bfloat16), ROWS_OF_BOTH, preferred_element_type=jnp.float32
    ).astype(jnp.bfloat16)
    for i in range(2):
        rows_ref[i, :, :512] = compressed[i * half : (i + 1) * half]
        rows_ref[i, :, 512:] = wide[i * half : (i + 1) * half]
    own_ref[...] = rows_ref[core_ref[0]]


def head_update(keys, query, values, scale, stat_ref, acc_ref, row, lo, hi, masks):
    scores = lax.dot_general(
        keys, query, (((1,), (1,)), ((), ())), preferred_element_type=jnp.float32
    ) * (scale * LOG2E)
    scores = masks(scores)
    old_top = stat_ref[row : row + 1, :]
    new_top = jnp.maximum(old_top, jnp.max(scores, axis=0, keepdims=True))
    weights = jnp.exp2(scores - new_top)
    factor = jnp.exp2(old_top - new_top)
    stat_ref[row : row + 1, :] = new_top
    stat_ref[row + 2 : row + 3, :] = stat_ref[row + 2 : row + 3, :] * factor + jnp.sum(
        weights, axis=0, keepdims=True
    )
    acc_ref[lo:hi, :] = acc_ref[lo:hi, :] * factor + jnp.dot(
        values, weights.astype(jnp.bfloat16), preferred_element_type=jnp.float32
    )


def chunk_update(piece, q_ref, wk_ref, wv_ref, stat_ref, acc_ref, scales, masks):
    keys = jnp.dot(piece[:, :512], wk_ref[...], preferred_element_type=jnp.float32)
    rope = piece[:, 512:].astype(jnp.float32)
    keys = jnp.concatenate(
        [keys[:, :128] + rope, keys[:, 128:256] + rope, keys[:, 256:]], axis=1
    ).astype(jnp.bfloat16)
    values = lax.dot_general(
        wv_ref[...], piece[:, :512], (((1,), (1,)), ((), ())), preferred_element_type=jnp.float32
    ).astype(jnp.bfloat16)
    head_update(
        keys[:, :128], q_ref[:, :128], values[:DV_A], scales[0], stat_ref, acc_ref,
        0, 0, DV_A, masks,
    )
    head_update(
        keys[:, 128:], q_ref[:, 128:], values[DV_A:], scales[1], stat_ref, acc_ref,
        1, DV_A, 256, masks,
    )


def own_kernel(
    scales, q_in, rope_in, cos_ref, sin_ref, wk_in, wv_ref, rows_ref,
    q_ref, wk_ref, stat_ref, acc_ref,
):
    turned = turn(rope_in[...], cos_ref, sin_ref)
    row = lax.broadcasted_iota(jnp.int32, (256, 384), 0)
    col = lax.broadcasted_iota(jnp.int32, (256, 384), 1)
    place = (col == jnp.where(row < DK_A, row + 32, row + 96)).astype(jnp.bfloat16)
    row = lax.broadcasted_iota(jnp.int32, (64, 384), 0)
    col = lax.broadcasted_iota(jnp.int32, (64, 384), 1)
    place_rope = (col == jnp.where(row < ROPE, row, row + 96)).astype(jnp.bfloat16)
    q_ref[...] = (
        jnp.dot(q_in[...], place, preferred_element_type=jnp.float32)
        + lax.dot_general(turned, place_rope, ROWS_OF_BOTH, preferred_element_type=jnp.float32)
    ).astype(jnp.bfloat16)
    wk_ref[...] = jnp.dot(wk_in[...], place, preferred_element_type=jnp.float32).astype(
        jnp.bfloat16
    )
    row = lax.broadcasted_iota(jnp.int32, stat_ref.shape, 0)
    stat_ref[...] = jnp.where(row < 2, floor_score, 0.0)
    acc_ref[...] = jnp.zeros(acc_ref.shape, jnp.float32)
    tokens = q_in.shape[0]

    def masks(scores):
        key_at = lax.broadcasted_iota(jnp.int32, (tokens, tokens), 0)
        query_at = lax.broadcasted_iota(jnp.int32, (tokens, tokens), 1)
        return jnp.where(query_at >= key_at, scores, floor_score)

    chunk_update(
        rows_ref[...].reshape(tokens, 640), q_ref, wk_ref, wv_ref, stat_ref, acc_ref, scales, masks
    )


def attend_kernel(scales, sizes, offsets, last, *refs):
    each, chunks = len(sizes), len(offsets)
    n, count = each * chunks, sum(sizes)
    info_ref = refs[0]
    shared_in = refs[1:6]
    piece_refs = refs[6 : 6 + n]
    if last:
        out_ref, buffer, sems, shared_sem, q_ref, wk_ref, wv_ref, stat_ref, acc_ref = refs[6 + n :]
    else:
        stat_ref, acc_ref, buffer, sems, shared_sem, q_ref, wk_ref, wv_ref = refs[6 + n :]
    rows = buffer.shape[2]

    def copy(i, k, piece_ref):
        low = sum(sizes[:k])
        if sizes[k] == 1:
            target = buffer.at[i, low]
        else:
            target = buffer.at[i, low : low + sizes[k]]
        return pltpu.make_async_copy(piece_ref, target, sems.at[i, k])

    shared = [
        pltpu.make_async_copy(src, dst, shared_sem.at[i])
        for i, (src, dst) in enumerate(zip(shared_in, (q_ref, wk_ref, wv_ref, stat_ref, acc_ref)))
    ]
    for c in shared:
        c.start()
    for i, piece_ref in enumerate(piece_refs):
        copy(i // each, i % each, piece_ref).start()
    for c in shared:
        c.wait()
    iy, ix, core = info_ref[0], info_ref[1], info_ref[2]
    own_index = iy * NX + ix

    def is_seen(i, k):
        flip, along, across = 0, 0, 0
        for j in range(chunks):
            f, a, c = offsets[j][k]
            hit = i == j
            flip = jnp.where(hit, f, flip)
            along = jnp.where(hit, a, along)
            across = jnp.where(hit, c, across)
        first_is_y = core == flip
        y = (iy + jnp.where(first_is_y, along, across) + NY) % NY
        x = (ix + jnp.where(first_is_y, across, along) + NX) % NX
        return y * NX + x < own_index

    def chunk(i, carry):
        for k in range(each):
            copy(i, k, piece_refs[k]).wait()
        seen = [is_seen(i, k) for k in range(count)]

        def masks(scores):
            return jnp.concatenate(
                [
                    jnp.where(v, scores[k * rows : (k + 1) * rows], floor_score)
                    for k, v in enumerate(seen)
                ],
                axis=0,
            )

        @pl.when(functools.reduce(jnp.logical_or, seen))
        def _():
            chunk_update(
                buffer[i].reshape(count * rows, 640),
                q_ref, wk_ref, wv_ref, stat_ref, acc_ref, scales, masks,
            )

        return carry

    lax.fori_loop(0, chunks, chunk, 0)
    if last:
        acc_ref[:DV_A, :] = acc_ref[:DV_A, :] / stat_ref[2:3, :]
        acc_ref[DV_A:, :] = acc_ref[DV_A:, :] / stat_ref[3:4, :]
        out_ref[...] = acc_ref[...].T.reshape(out_ref.shape).astype(jnp.bfloat16)


VMEM = pl.BlockSpec(memory_space=pltpu.VMEM)
HBM = pl.BlockSpec(memory_space=pltpu.MemorySpace.HBM)


def fetched(kernel, scalars, arrays):
    n = len(arrays)

    def body(*refs):
        heads, sources = refs[:scalars], refs[scalars : scalars + n]
        rest, buffers, sems = refs[scalars + n : -n - 1], refs[-n - 1 : -1], refs[-1]
        copies = [
            pltpu.make_async_copy(src, dst, sems.at[i])
            for i, (src, dst) in enumerate(zip(sources, buffers))
        ]
        for c in copies:
            c.start()
        for c in copies:
            c.wait()
        kernel(*heads, *buffers, *rest)

    scratch = [pltpu.VMEM(a.shape, a.dtype) for a in arrays]
    return body, [HBM] * n, scratch + [pltpu.SemaphoreType.DMA((n,))]


ANY = pl.BlockSpec(memory_space=pl.ANY)
SMEM = pl.BlockSpec(memory_space=pltpu.SMEM)
PARAMS = pltpu.CompilerParams(vmem_limit_bytes=20 * 1024 * 1024)
LARGE = pltpu.CompilerParams(vmem_limit_bytes=67_043_328)


def attend(info, offsets, pieces, q, wk, wv, state, last, scales):
    n, chunks = len(pieces), len(offsets)
    each = n // chunks
    sizes = tuple(1 if p.ndim == 2 else p.shape[0] for p in pieces[:each])
    rows = pieces[0].shape[-2]
    tokens = q.shape[0]
    stat = jax.ShapeDtypeStruct((8, tokens), jnp.float32)
    acc = jax.ShapeDtypeStruct((256, tokens), jnp.float32)
    if last:
        out_shape = jax.ShapeDtypeStruct((NZ * NC, tokens // (NZ * NC), 256), jnp.bfloat16)
        out_specs = VMEM
        scratch = [pltpu.VMEM(stat.shape, stat.dtype), pltpu.VMEM(acc.shape, acc.dtype)]
    else:
        out_shape = (stat, acc)
        out_specs = (VMEM, VMEM)
        scratch = []
    scratch = [
        pltpu.VMEM((chunks, sum(sizes), rows, 640), pieces[0].dtype),
        pltpu.SemaphoreType.DMA((chunks, each)),
        pltpu.SemaphoreType.DMA((5,)),
        *[pltpu.VMEM(v.shape, v.dtype) for v in (q, wk, wv)],
    ] + scratch
    total = chunks * sum(sizes) * rows
    return pl.pallas_call(
        functools.partial(attend_kernel, scales, sizes, offsets, last),
        in_specs=[SMEM] + [HBM] * (5 + n),
        out_specs=out_specs,
        out_shape=out_shape,
        scratch_shapes=scratch,
        cost_estimate=pl.CostEstimate(
            flops=2 * total * (640 * 384 + 512 * 256 + tokens * 640),
            bytes_accessed=total * 1280,
            transcendentals=2 * total * tokens,
        ),
        compiler_params=LARGE,
        name="attend",
    )(info, q, wk, wv, *state, *pieces)


def project_kernel(info_ref, own_ref, other_ref, w_own_ref, w_other_ref, *out_refs):
    def rows(ref):
        return jnp.concatenate(
            [ref[info_ref[i]].astype(jnp.float32) for i in range(8)], axis=0
        ).astype(jnp.bfloat16)

    out = jnp.dot(rows(own_ref), w_own_ref[...], preferred_element_type=jnp.float32) + jnp.dot(
        rows(other_ref), w_other_ref[...], preferred_element_type=jnp.float32
    )
    low = 0
    for ref in out_refs:
        high = low + ref.shape[0]
        ref[...] = out[low:high].astype(ref.dtype)
        low = high


def stack_kernel(a_ref, b_ref, out_ref, sems):
    copies = [
        pltpu.make_async_copy(ref, out_ref.at[i], sems.at[i]) for i, ref in enumerate((a_ref, b_ref))
    ]
    for c in copies:
        c.start()
    for c in copies:
        c.wait()


def stack_of(a, b):
    return pl.pallas_call(
        stack_kernel,
        in_specs=[HBM, HBM],
        out_specs=VMEM,
        out_shape=jax.ShapeDtypeStruct((2, *a.shape), a.dtype),
        scratch_shapes=[pltpu.SemaphoreType.DMA((2,))],
        cost_estimate=pl.CostEstimate(flops=1 << 20, bytes_accessed=4 * a.size, transcendentals=0),
        compiler_params=LARGE,
        name="stack",
    )(a, b)


def hidden_kernel(n, *refs):
    block_refs = refs[: 2 * n]
    gate_ref, up_ref, keep_ref, give_ref = refs[2 * n :]
    per = block_refs[0].shape[0] // 2

    def expert(e, carry):
        at = pl.ds(pl.multiple_of(e * per, per), per)
        stacked = jnp.concatenate([ref[at, :] for ref in block_refs], axis=0)
        gate_out = jnp.dot(stacked, gate_ref[e], preferred_element_type=jnp.float32)
        up_out = jnp.dot(stacked, up_ref[e], preferred_element_type=jnp.float32)
        hidden = (gate_out / (1.0 + jnp.exp(-gate_out)) * up_out).astype(jnp.bfloat16)
        keep_ref[e] = hidden[: n * per]
        give_ref[e] = hidden[n * per :]
        return carry

    lax.fori_loop(0, 2, expert, 0)


def slot_table(route_block, experts_all, capacity):
    flat_routes = route_block.reshape(-1)
    onehot = (flat_routes[:, None] == jnp.arange(experts_all, dtype=jnp.int32)[None, :]).astype(
        jnp.int32
    )
    rank_within = jnp.sum((jnp.cumsum(onehot, axis=0) - onehot) * onehot, axis=1)
    return flat_routes * capacity + rank_within


def layer(
    residual,
    queries,
    query_rope,
    latent,
    key_rope,
    latent_gain,
    key_weight,
    value_weight,
    out_weight,
    norm_gain,
    routes,
    group_gate,
    expert_share,
    gate_weight,
    up_weight,
    down_weight,
):
    tokens = queries.shape[0]
    half_rows = tokens // 2
    row_count = residual.shape[0]
    width = residual.shape[1]
    iy, ix, iz, core = (lax.axis_index(a) for a in AXES)
    index = iy * NX + ix
    first_place = index * tokens
    places = (first_place + jnp.arange(tokens, dtype=jnp.int32)).astype(jnp.float32)
    frequencies = rope_base ** (-jnp.arange(0, ROPE, 2, dtype=jnp.float32) / ROPE)
    angles = places[None, :] * frequencies[:, None]
    cosine, sine = jnp.cos(angles), jnp.sin(angles)
    latent_args = (latent, latent_gain[None], key_rope.T, cosine, sine)
    body, specs, scratch = fetched(latent_kernel, 1, latent_args)
    rows, own_piece = pl.pallas_call(
        body,
        in_specs=[SMEM] + specs,
        out_specs=(VMEM, VMEM),
        out_shape=(
            jax.ShapeDtypeStruct((2, half_rows, 640), jnp.bfloat16),
            jax.ShapeDtypeStruct((half_rows, 640), jnp.bfloat16),
        ),
        scratch_shapes=scratch,
        compiler_params=LARGE,
        name="latent_rows",
    )(core[None], *latent_args)

    out_other = swap(out_weight[0])
    down_other = swap(down_weight)

    wv = value_weight[:, 0].T
    scales = ((DK_A + ROPE) ** (-0.5), (queries.shape[2] - DK_A + ROPE) ** (-0.5))

    other = 1 - core
    info = jnp.stack([iy, ix, core]).astype(jnp.int32)

    behind = send(own_piece, first_axis(1))
    ahead = send(own_piece, first_axis(-1))
    across = send(own_piece, first_axis(2))
    own_args = (
        queries[:, 0], query_rope[:, 0].T, cosine, sine, key_weight[:, 0], wv, rows,
    )
    body, specs, scratch = fetched(functools.partial(own_kernel, scales), 0, own_args)
    q, wk, *state = pl.pallas_call(
        body,
        in_specs=specs,
        out_specs=[VMEM] * 4,
        out_shape=[
            jax.ShapeDtypeStruct((tokens, 384), jnp.bfloat16),
            jax.ShapeDtypeStruct((512, 384), jnp.bfloat16),
            jax.ShapeDtypeStruct((8, tokens), jnp.float32),
            jax.ShapeDtypeStruct((256, tokens), jnp.float32),
        ],
        scratch_shapes=scratch,
        cost_estimate=pl.CostEstimate(
            flops=2 * tokens * (640 * 384 + 512 * 256 + tokens * 640),
            bytes_accessed=tokens * 1280,
            transcendentals=2 * tokens * tokens,
        ),
        compiler_params=LARGE,
        name="attend_own",
    )(*own_args)
    near = stack_of(own_piece, behind)
    side = stack_of(ahead, across)
    near_behind = send(near, second_axis(1))
    side_ahead = send(side, second_axis(-1))
    side_behind = send(side, second_axis(1))
    near_ahead = send(near, second_axis(-1))
    behind_swap = swap(behind)
    side_swap = swap(side)
    order = (0, -1, 1, 2)

    def lie(flip, along, across):
        return tuple((flip, step, across) for step in along)

    state = attend(
        info, (lie(0, order[1:], 0), lie(1, order[1:], 0)),
        [behind, side, behind_swap, side_swap],
        q, wk, wv, state, False, scales,
    )
    far_low = send(near_behind, second_axis(1))
    far_high = send(side_ahead, second_axis(-1))
    arrived = [near_behind, side_behind, near_ahead, side_ahead]
    swapped = []
    for value in arrived:
        swapped.append(swap(value))
    state = attend(
        info, (lie(0, order, -1), lie(0, order, 1), lie(1, order, -1), lie(1, order, 1)),
        arrived + swapped,
        q, wk, wv, state, False, scales,
    )
    low_swap = swap(far_low)
    high_swap = swap(far_high)
    attention = attend(
        info, (lie(0, order, 2), lie(1, order, 2)),
        [far_low, far_high, low_swap, high_swap],
        q, wk, wv, state, True, scales,
    )

    attention_other = swap(attention)
    way = jnp.where(core == 0, -1, 1)
    blocks = []
    for k in (1, 2, 3):
        blocks += [(iz + way * k) % NZ * NC + core, (iz + way * k) % NZ * NC + other]
    blocks += [(iz + 4) % NZ * NC + core, iz * NC + core]
    low, wide = jnp.bfloat16, jnp.float32
    types = [wide, wide, wide, wide, wide, low, low, wide]
    project_args = (attention, attention_other, out_weight[0], out_other)
    body, specs, scratch = fetched(project_kernel, 1, project_args)
    a_m1, a_p1, a_m2, a_p2, a_m3, a_p3, a_m4, here = pl.pallas_call(
        body,
        in_specs=[SMEM] + specs,
        scratch_shapes=scratch,
        out_specs=[VMEM] * 8,
        out_shape=[jax.ShapeDtypeStruct((row_count, width), t) for t in types],
        cost_estimate=pl.CostEstimate(
            flops=2 * 192 * 512 * width, bytes_accessed=4 * 512 * width, transcendentals=0
        ),
        compiler_params=LARGE,
        name="project",
    )(jnp.stack(blocks).astype(jnp.int32), *project_args)
    onward = ring(1)
    back = ring(-1)

    def hop(value, addend):
        return (send(value, back).astype(wide) + addend).astype(low)

    head_m = hop(a_m4, a_m3)
    head_p = hop(a_p3, a_p2)
    head_m = hop(head_m, a_m2)
    head_p = hop(head_p, a_p1)
    head_m = hop(head_m, a_m1)
    head_p = swap(send(head_p, back))
    head_m = send(head_m, back)
    head_total = here + head_m.astype(wide) + head_p.astype(wide)
    mixed_rows = residual.astype(jnp.float32) + head_total
    normed = rms_scale(mixed_rows, norm_gain).astype(jnp.bfloat16)

    experts_dev = gate_weight.shape[0]
    sp_count = NY * NX
    experts_all = experts_dev * sp_count
    top_count = routes.shape[1]
    slot_count = experts_all * CAP
    own_routes = lax.dynamic_slice_in_dim(routes, (iz * NC + core) * row_count, row_count, 0)
    own_slots = slot_table(own_routes, experts_all, CAP)
    pick_matrix = (
        jnp.arange(slot_count, dtype=jnp.int32)[:, None] == own_slots[None, :]
    ).astype(jnp.bfloat16)
    pick_matrix = pick_matrix.reshape(slot_count, row_count, top_count).sum(axis=2)
    outgoing = jnp.dot(pick_matrix, normed, preferred_element_type=jnp.float32).astype(jnp.bfloat16)
    arrived_rows = lax.all_to_all(
        outgoing.reshape(sp_count, experts_dev * CAP, width), SP, 0, 0, tiled=True
    ).reshape(slot_count, width)
    slot = jnp.arange(slot_count, dtype=jnp.int32)
    per = sp_count * CAP
    source = (slot % per) // CAP * (experts_dev * CAP) + slot // per * CAP + slot % CAP
    shuffle = (source[:, None] == slot[None, :]).astype(jnp.bfloat16)
    own = jnp.dot(shuffle, arrived_rows, preferred_element_type=jnp.float32).astype(jnp.bfloat16)

    block_bytes = slot_count * width * 2

    def hidden_of(mine, theirs):
        n = len(mine)
        shape = jax.ShapeDtypeStruct((experts_dev, n * per, gate_weight.shape[2]), jnp.bfloat16)
        keep, give = pl.pallas_call(
            functools.partial(hidden_kernel, n),
            in_specs=[VMEM] * (2 * n + 2),
            out_specs=[VMEM] * 2,
            out_shape=[shape] * 2,
            cost_estimate=pl.CostEstimate(
                flops=2 * 2 * n * slot_count * width * 512,
                bytes_accessed=2 * n * block_bytes + 4 * width * 512 * 2,
                transcendentals=2 * n * slot_count * 256,
            ),
            compiler_params=PARAMS,
            name="hidden",
        )(*mine, *theirs, gate_weight, up_weight)
        return keep, give

    def outputs_of(keep, got, types):
        result = [
            jnp.dot(keep[e], down_weight[e], preferred_element_type=wide)
            + jnp.dot(got[e], down_other[e], preferred_element_type=wide)
            for e in range(experts_dev)
        ]
        return [
            jnp.concatenate([r[i * per : (i + 1) * per] for r in result], axis=0).astype(t)
            for i, t in enumerate(types)
        ]

    m1 = send(own, onward)
    par = swap(own)
    p1 = send(par, onward)
    h0 = hidden_of([own], [par])
    m2 = send(m1, onward)
    sm1 = swap(m1)
    p2 = send(p1, onward)
    sp1 = swap(p1)
    h1 = hidden_of([m1, p1], [sm1, sp1])
    m3 = send(m2, onward)
    sm2 = swap(m2)
    p3 = send(p2, onward)
    sp2 = swap(p2)
    h2 = hidden_of([m2, p2], [sm2, sp2])
    m4 = send(m3, onward)
    sm3 = swap(m3)
    sp3 = swap(p3)
    h3 = hidden_of([m3, p3], [sm3, sp3])
    sm4 = swap(m4)
    h4 = hidden_of([m4], [sm4])
    o_m3, o_p3 = outputs_of(h3[0], swap(h3[1]), (wide, wide))
    (o_m4,) = outputs_of(h4[0], swap(h4[1]), (low,))
    keep, give = (jnp.concatenate(h, axis=1) for h in zip(h0, h1, h2))
    got = swap(give)
    o_own, o_m1, o_p1, o_m2, o_p2 = outputs_of(keep, got, (wide,) * 5)

    chain_p = hop(o_p3.astype(low), o_p2)
    chain_m = hop(o_m4, o_m3)
    chain_p = hop(chain_p, o_p1)
    chain_m = hop(chain_m, o_m2)
    chain_p = swap(send(chain_p, back))
    chain_m = hop(chain_m, o_m1)
    chain_m = send(chain_m, back)
    total = (o_own + chain_m.astype(wide) + chain_p.astype(wide)).astype(low)

    unshuffled = lax.dot_general(
        shuffle, total, (((0,), (0,)), ((), ())), preferred_element_type=jnp.float32
    ).astype(jnp.bfloat16)
    returned = lax.all_to_all(
        unshuffled.reshape(sp_count, experts_dev * CAP, width), SP, 0, 0, tiled=True
    ).reshape(slot_count, width)
    selectors = (own_slots[:, None] == slot[None, :]).astype(jnp.bfloat16)
    picked = jnp.dot(selectors, returned, preferred_element_type=jnp.float32).reshape(
        row_count, top_count, -1
    )
    route_weight = group_gate[:, None] * expert_share / jnp.sum(expert_share, axis=1, keepdims=True)
    expert_mix = jnp.sum(route_weight[:, :, None] * picked, axis=1)
    return (mixed_rows + expert_mix).astype(jnp.bfloat16)


def solution(mesh):
    finer = Mesh(mesh.devices.reshape(NY, NX, NZ, NC), AXES)
    tp = ("z", "c")
    placed = (
        P(AXES, None),
        P(SP, tp, None),
        P(SP, tp, None),
        P(SP, None),
        P(SP, None),
        P(),
        P(None, tp, None),
        P(None, tp, None),
        P(tp, None, None),
        P(),
        P(SP, None),
        P(AXES),
        P(AXES, None),
        P(SP, None, tp),
        P(SP, None, tp),
        P(SP, tp, None),
    )
    return jax.shard_map(
        layer, mesh=finer, in_specs=placed, out_specs=P(AXES, None), check_vma=False
    )
```

```python
import functools

import jax
import jax.numpy as jnp
from jax import lax
from jax.experimental import pallas as pl
from jax.experimental.pallas import tpu as pltpu
from jax.sharding import Mesh
from jax.sharding import PartitionSpec as P


AXES = ("y", "x", "z", "c")
SP = ("y", "x")
NY, NX, NZ, NC = 4, 4, 8, 2
DK_A = 64
DV_A = 64
ROPE = 32
CAP = 2
LOG2E = 1.4426950408889634

rope_base = 10000.0
epsilon = 1e-06
floor_score = -1e30


def flat(y, x, z, c):
    return ((y * NX + x) * NZ + z) * NC + c


def moves(target):
    pairs = []
    for y in range(NY):
        for x in range(NX):
            for z in range(NZ):
                for c in range(NC):
                    pairs.append((flat(y, x, z, c), flat(*target(y, x, z, c))))
    return pairs


def first_axis(step):
    return moves(
        lambda y, x, z, c: ((y + step) % NY, x, z, c) if c == 0 else (y, (x + step) % NX, z, c)
    )


def second_axis(step):
    return moves(
        lambda y, x, z, c: (y, (x + step) % NX, z, c) if c == 0 else ((y + step) % NY, x, z, c)
    )


def ring(sign):
    return moves(lambda y, x, z, c: (y, x, (z + (sign if c == 0 else -sign)) % NZ, c))


PARTNER = moves(lambda y, x, z, c: (y, x, z, 1 - c))


def send(value, pairs):
    return lax.ppermute(value, AXES, pairs)


def swap(value):
    return lax.ppermute(value, AXES, PARTNER)


def rms_scale(values, gain_vector):
    values = values.astype(jnp.float32)
    inverse = lax.rsqrt(jnp.mean(values * values, axis=-1, keepdims=True) + epsilon)
    return values * inverse * gain_vector


def turn(values, cos_ref, sin_ref):
    cosine, sine = cos_ref[...], sin_ref[...]
    values = values.astype(jnp.float32)
    out = []
    for lo in range(0, values.shape[0], ROPE):
        u = values[lo : lo + ROPE // 2]
        w = values[lo + ROPE // 2 : lo + ROPE]
        out += [u * cosine - w * sine, w * cosine + u * sine]
    return jnp.concatenate(out, axis=0).astype(jnp.bfloat16)


ROWS_OF_BOTH = (((0,), (0,)), ((), ()))


def latent_kernel(core_ref, latent_ref, gain_ref, rope_ref, cos_ref, sin_ref, rows_ref, own_ref):
    half = latent_ref.shape[0] // 2
    compressed = rms_scale(latent_ref[...], gain_ref[...]).astype(jnp.bfloat16)
    turned = turn(rope_ref[...], cos_ref, sin_ref)
    row = lax.broadcasted_iota(jnp.int32, (ROPE, 128), 0)
    col = lax.broadcasted_iota(jnp.int32, (ROPE, 128), 1)
    wide = lax.dot_general(
        turned, (row == col).astype(jnp.bfloat16), ROWS_OF_BOTH, preferred_element_type=jnp.float32
    ).astype(jnp.bfloat16)
    for i in range(2):
        rows_ref[i, :, :512] = compressed[i * half : (i + 1) * half]
        rows_ref[i, :, 512:] = wide[i * half : (i + 1) * half]
    own_ref[...] = rows_ref[core_ref[0]]


def head_update(keys, query, values, scale, stat_ref, acc_ref, row, lo, hi, masks):
    scores = lax.dot_general(
        keys, query, (((1,), (1,)), ((), ())), preferred_element_type=jnp.float32
    ) * (scale * LOG2E)
    scores = masks(scores)
    old_top = stat_ref[row : row + 1, :]
    new_top = jnp.maximum(old_top, jnp.max(scores, axis=0, keepdims=True))
    weights = jnp.exp2(scores - new_top)
    factor = jnp.exp2(old_top - new_top)
    stat_ref[row : row + 1, :] = new_top
    stat_ref[row + 2 : row + 3, :] = stat_ref[row + 2 : row + 3, :] * factor + jnp.sum(
        weights, axis=0, keepdims=True
    )
    acc_ref[lo:hi, :] = acc_ref[lo:hi, :] * factor + jnp.dot(
        values, weights.astype(jnp.bfloat16), preferred_element_type=jnp.float32
    )


def chunk_update(piece, q_ref, wk_ref, wv_ref, stat_ref, acc_ref, scales, masks):
    keys = jnp.dot(piece[:, :512], wk_ref[...], preferred_element_type=jnp.float32)
    rope = piece[:, 512:].astype(jnp.float32)
    keys = jnp.concatenate(
        [keys[:, :128] + rope, keys[:, 128:256] + rope, keys[:, 256:]], axis=1
    ).astype(jnp.bfloat16)
    values = lax.dot_general(
        wv_ref[...], piece[:, :512], (((1,), (1,)), ((), ())), preferred_element_type=jnp.float32
    ).astype(jnp.bfloat16)
    head_update(
        keys[:, :128], q_ref[:, :128], values[:DV_A], scales[0], stat_ref, acc_ref,
        0, 0, DV_A, masks,
    )
    head_update(
        keys[:, 128:], q_ref[:, 128:], values[DV_A:], scales[1], stat_ref, acc_ref,
        1, DV_A, 256, masks,
    )


def own_kernel(
    scales, q_in, rope_in, cos_ref, sin_ref, wk_in, wv_ref, rows_ref,
    q_ref, wk_ref, stat_ref, acc_ref,
):
    turned = turn(rope_in[...], cos_ref, sin_ref)
    row = lax.broadcasted_iota(jnp.int32, (256, 384), 0)
    col = lax.broadcasted_iota(jnp.int32, (256, 384), 1)
    place = (col == jnp.where(row < DK_A, row + 32, row + 96)).astype(jnp.bfloat16)
    row = lax.broadcasted_iota(jnp.int32, (64, 384), 0)
    col = lax.broadcasted_iota(jnp.int32, (64, 384), 1)
    place_rope = (col == jnp.where(row < ROPE, row, row + 96)).astype(jnp.bfloat16)
    q_ref[...] = (
        jnp.dot(q_in[...], place, preferred_element_type=jnp.float32)
        + lax.dot_general(turned, place_rope, ROWS_OF_BOTH, preferred_element_type=jnp.float32)
    ).astype(jnp.bfloat16)
    wk_ref[...] = jnp.dot(wk_in[...], place, preferred_element_type=jnp.float32).astype(
        jnp.bfloat16
    )
    row = lax.broadcasted_iota(jnp.int32, stat_ref.shape, 0)
    stat_ref[...] = jnp.where(row < 2, floor_score, 0.0)
    acc_ref[...] = jnp.zeros(acc_ref.shape, jnp.float32)
    tokens = q_in.shape[0]

    def masks(scores):
        key_at = lax.broadcasted_iota(jnp.int32, (tokens, tokens), 0)
        query_at = lax.broadcasted_iota(jnp.int32, (tokens, tokens), 1)
        return jnp.where(query_at >= key_at, scores, floor_score)

    chunk_update(
        rows_ref[...].reshape(tokens, 640), q_ref, wk_ref, wv_ref, stat_ref, acc_ref, scales, masks
    )


def attend_kernel(scales, sizes, offsets, last, *refs):
    each, chunks = len(sizes), len(offsets)
    n, count = each * chunks, sum(sizes)
    info_ref = refs[0]
    shared_in = refs[1:6]
    piece_refs = refs[6 : 6 + n]
    if last:
        out_ref, buffer, sems, shared_sem, q_ref, wk_ref, wv_ref, stat_ref, acc_ref = refs[6 + n :]
    else:
        stat_ref, acc_ref, buffer, sems, shared_sem, q_ref, wk_ref, wv_ref = refs[6 + n :]
    rows = buffer.shape[2]

    def copy(i, k, piece_ref):
        low = sum(sizes[:k])
        if sizes[k] == 1:
            target = buffer.at[i, low]
        else:
            target = buffer.at[i, low : low + sizes[k]]
        return pltpu.make_async_copy(piece_ref, target, sems.at[i, k])

    shared = [
        pltpu.make_async_copy(src, dst, shared_sem.at[i])
        for i, (src, dst) in enumerate(zip(shared_in, (q_ref, wk_ref, wv_ref, stat_ref, acc_ref)))
    ]
    for c in shared:
        c.start()
    for i, piece_ref in enumerate(piece_refs):
        copy(i // each, i % each, piece_ref).start()
    for c in shared:
        c.wait()
    iy, ix, core = info_ref[0], info_ref[1], info_ref[2]
    own_index = iy * NX + ix

    def is_seen(i, k):
        flip, along, across = 0, 0, 0
        for j in range(chunks):
            f, a, c = offsets[j][k]
            hit = i == j
            flip = jnp.where(hit, f, flip)
            along = jnp.where(hit, a, along)
            across = jnp.where(hit, c, across)
        first_is_y = core == flip
        y = (iy + jnp.where(first_is_y, along, across) + NY) % NY
        x = (ix + jnp.where(first_is_y, across, along) + NX) % NX
        return y * NX + x < own_index

    def chunk(i, carry):
        for k in range(each):
            copy(i, k, piece_refs[k]).wait()
        seen = [is_seen(i, k) for k in range(count)]

        def masks(scores):
            return jnp.concatenate(
                [
                    jnp.where(v, scores[k * rows : (k + 1) * rows], floor_score)
                    for k, v in enumerate(seen)
                ],
                axis=0,
            )

        @pl.when(functools.reduce(jnp.logical_or, seen))
        def _():
            chunk_update(
                buffer[i].reshape(count * rows, 640),
                q_ref, wk_ref, wv_ref, stat_ref, acc_ref, scales, masks,
            )

        return carry

    lax.fori_loop(0, chunks, chunk, 0)
    if last:
        acc_ref[:DV_A, :] = acc_ref[:DV_A, :] / stat_ref[2:3, :]
        acc_ref[DV_A:, :] = acc_ref[DV_A:, :] / stat_ref[3:4, :]
        out_ref[...] = acc_ref[...].T.reshape(out_ref.shape).astype(jnp.bfloat16)


VMEM = pl.BlockSpec(memory_space=pltpu.VMEM)
HBM = pl.BlockSpec(memory_space=pltpu.MemorySpace.HBM)


def fetched(kernel, scalars, arrays):
    n = len(arrays)

    def body(*refs):
        heads, sources = refs[:scalars], refs[scalars : scalars + n]
        rest, buffers, sems = refs[scalars + n : -n - 1], refs[-n - 1 : -1], refs[-1]
        copies = [
            pltpu.make_async_copy(src, dst, sems.at[i])
            for i, (src, dst) in enumerate(zip(sources, buffers))
        ]
        for c in copies:
            c.start()
        for c in copies:
            c.wait()
        kernel(*heads, *buffers, *rest)

    scratch = [pltpu.VMEM(a.shape, a.dtype) for a in arrays]
    return body, [HBM] * n, scratch + [pltpu.SemaphoreType.DMA((n,))]


ANY = pl.BlockSpec(memory_space=pl.ANY)
SMEM = pl.BlockSpec(memory_space=pltpu.SMEM)
PARAMS = pltpu.CompilerParams(vmem_limit_bytes=20 * 1024 * 1024)
LARGE = pltpu.CompilerParams(vmem_limit_bytes=67_043_328)


def attend(info, offsets, pieces, q, wk, wv, state, last, scales):
    n, chunks = len(pieces), len(offsets)
    each = n // chunks
    sizes = tuple(1 if p.ndim == 2 else p.shape[0] for p in pieces[:each])
    rows = pieces[0].shape[-2]
    tokens = q.shape[0]
    stat = jax.ShapeDtypeStruct((8, tokens), jnp.float32)
    acc = jax.ShapeDtypeStruct((256, tokens), jnp.float32)
    if last:
        out_shape = jax.ShapeDtypeStruct((NZ * NC, tokens // (NZ * NC), 256), jnp.bfloat16)
        out_specs = VMEM
        scratch = [pltpu.VMEM(stat.shape, stat.dtype), pltpu.VMEM(acc.shape, acc.dtype)]
    else:
        out_shape = (stat, acc)
        out_specs = (VMEM, VMEM)
        scratch = []
    scratch = [
        pltpu.VMEM((chunks, sum(sizes), rows, 640), pieces[0].dtype),
        pltpu.SemaphoreType.DMA((chunks, each)),
        pltpu.SemaphoreType.DMA((5,)),
        *[pltpu.VMEM(v.shape, v.dtype) for v in (q, wk, wv)],
    ] + scratch
    total = chunks * sum(sizes) * rows
    return pl.pallas_call(
        functools.partial(attend_kernel, scales, sizes, offsets, last),
        in_specs=[SMEM] + [HBM] * (5 + n),
        out_specs=out_specs,
        out_shape=out_shape,
        scratch_shapes=scratch,
        cost_estimate=pl.CostEstimate(
            flops=2 * total * (640 * 384 + 512 * 256 + tokens * 640),
            bytes_accessed=total * 1280,
            transcendentals=2 * total * tokens,
        ),
        compiler_params=LARGE,
        name="attend",
    )(info, q, wk, wv, *state, *pieces)


def project_kernel(info_ref, own_ref, other_ref, w_own_ref, w_other_ref, *out_refs):
    core, iz = info_ref[2], info_ref[3]
    way = jnp.where(core == 0, -1, 1)
    blocks = []
    for k in (1, 2, 3):
        chip = (iz + NZ + way * k) % NZ
        blocks += [chip * NC + core, chip * NC + 1 - core]
    blocks += [(iz + 4) % NZ * NC + core, iz * NC + core]

    def rows(ref):
        return jnp.concatenate(
            [ref[i].astype(jnp.float32) for i in blocks], axis=0
        ).astype(jnp.bfloat16)

    out = jnp.dot(rows(own_ref), w_own_ref[...], preferred_element_type=jnp.float32) + jnp.dot(
        rows(other_ref), w_other_ref[...], preferred_element_type=jnp.float32
    )
    low = 0
    for ref in out_refs:
        high = low + ref.shape[0]
        ref[...] = out[low:high].astype(ref.dtype)
        low = high


def join_kernel(low_ref, high_ref, out_ref, sems):
    half = low_ref.shape[1]
    copies = [
        pltpu.make_async_copy(low_ref, out_ref.at[:, :half], sems.at[0]),
        pltpu.make_async_copy(high_ref, out_ref.at[:, half:], sems.at[1]),
    ]
    for c in copies:
        c.start()
    for c in copies:
        c.wait()


def stack_kernel(a_ref, b_ref, out_ref, sems):
    copies = [
        pltpu.make_async_copy(ref, out_ref.at[i], sems.at[i]) for i, ref in enumerate((a_ref, b_ref))
    ]
    for c in copies:
        c.start()
    for c in copies:
        c.wait()


def stack_of(a, b):
    return pl.pallas_call(
        stack_kernel,
        in_specs=[HBM, HBM],
        out_specs=VMEM,
        out_shape=jax.ShapeDtypeStruct((2, *a.shape), a.dtype),
        scratch_shapes=[pltpu.SemaphoreType.DMA((2,))],
        cost_estimate=pl.CostEstimate(flops=1 << 20, bytes_accessed=4 * a.size, transcendentals=0),
        compiler_params=LARGE,
        name="stack",
    )(a, b)


def hidden_kernel(n, *refs):
    block_refs = refs[: 2 * n]
    gate_ref, up_ref, keep_ref, give_ref = refs[2 * n :]
    per = block_refs[0].shape[0] // 2

    def expert(e, carry):
        at = pl.ds(pl.multiple_of(e * per, per), per)
        stacked = jnp.concatenate([ref[at, :] for ref in block_refs], axis=0)
        gate_out = jnp.dot(stacked, gate_ref[e], preferred_element_type=jnp.float32)
        up_out = jnp.dot(stacked, up_ref[e], preferred_element_type=jnp.float32)
        hidden = (gate_out / (1.0 + jnp.exp(-gate_out)) * up_out).astype(jnp.bfloat16)
        keep_ref[e] = hidden[: n * per]
        give_ref[e] = hidden[n * per :]
        return carry

    lax.fori_loop(0, 2, expert, 0)


def slot_table(route_block, experts_all, capacity):
    flat_routes = route_block.reshape(-1)
    onehot = (flat_routes[:, None] == jnp.arange(experts_all, dtype=jnp.int32)[None, :]).astype(
        jnp.int32
    )
    rank_within = jnp.sum((jnp.cumsum(onehot, axis=0) - onehot) * onehot, axis=1)
    return flat_routes * capacity + rank_within


def layer(
    residual,
    queries,
    query_rope,
    latent,
    key_rope,
    latent_gain,
    key_weight,
    value_weight,
    out_weight,
    norm_gain,
    routes,
    group_gate,
    expert_share,
    gate_weight,
    up_weight,
    down_weight,
):
    tokens = queries.shape[0]
    half_rows = tokens // 2
    row_count = residual.shape[0]
    width = residual.shape[1]
    iy, ix, iz, core = (lax.axis_index(a) for a in AXES)
    index = iy * NX + ix
    first_place = index * tokens
    places = (first_place + jnp.arange(tokens, dtype=jnp.int32)).astype(jnp.float32)
    frequencies = rope_base ** (-jnp.arange(0, ROPE, 2, dtype=jnp.float32) / ROPE)
    angles = places[None, :] * frequencies[:, None]
    cosine, sine = jnp.cos(angles), jnp.sin(angles)
    latent_args = (latent, latent_gain[None], key_rope.T, cosine, sine)
    body, specs, scratch = fetched(latent_kernel, 1, latent_args)
    rows, own_piece = pl.pallas_call(
        body,
        in_specs=[SMEM] + specs,
        out_specs=(VMEM, VMEM),
        out_shape=(
            jax.ShapeDtypeStruct((2, half_rows, 640), jnp.bfloat16),
            jax.ShapeDtypeStruct((half_rows, 640), jnp.bfloat16),
        ),
        scratch_shapes=scratch,
        compiler_params=LARGE,
        name="latent_rows",
    )(core[None], *latent_args)

    out_other = swap(out_weight[0])
    down_other = swap(down_weight)

    wv = value_weight[:, 0].T
    scales = ((DK_A + ROPE) ** (-0.5), (queries.shape[2] - DK_A + ROPE) ** (-0.5))

    info = jnp.stack([iy, ix, core, iz]).astype(jnp.int32)

    behind = send(own_piece, first_axis(1))
    ahead = send(own_piece, first_axis(-1))
    across = send(own_piece, first_axis(2))
    own_args = (
        queries[:, 0], query_rope[:, 0].T, cosine, sine, key_weight[:, 0], wv, rows,
    )
    body, specs, scratch = fetched(functools.partial(own_kernel, scales), 0, own_args)
    q, wk, *state = pl.pallas_call(
        body,
        in_specs=specs,
        out_specs=[VMEM] * 4,
        out_shape=[
            jax.ShapeDtypeStruct((tokens, 384), jnp.bfloat16),
            jax.ShapeDtypeStruct((512, 384), jnp.bfloat16),
            jax.ShapeDtypeStruct((8, tokens), jnp.float32),
            jax.ShapeDtypeStruct((256, tokens), jnp.float32),
        ],
        scratch_shapes=scratch,
        cost_estimate=pl.CostEstimate(
            flops=2 * tokens * (640 * 384 + 512 * 256 + tokens * 640),
            bytes_accessed=tokens * 1280,
            transcendentals=2 * tokens * tokens,
        ),
        compiler_params=LARGE,
        name="attend_own",
    )(*own_args)
    near = stack_of(own_piece, behind)
    side = stack_of(ahead, across)
    near_behind = send(near, second_axis(1))
    side_ahead = send(side, second_axis(-1))
    side_behind = send(side, second_axis(1))
    near_ahead = send(near, second_axis(-1))
    behind_swap = swap(behind)
    side_swap = swap(side)
    order = (0, -1, 1, 2)

    def lie(flip, along, across):
        return tuple((flip, step, across) for step in along)

    state = attend(
        info, (lie(0, order[1:], 0), lie(1, order[1:], 0)),
        [behind, side, behind_swap, side_swap],
        q, wk, wv, state, False, scales,
    )
    far_low = send(near_behind, second_axis(1))
    far_high = send(side_ahead, second_axis(-1))
    arrived = [near_behind, side_behind, near_ahead, side_ahead]
    swapped = []
    for value in arrived:
        swapped.append(swap(value))
    state = attend(
        info, (lie(0, order, -1), lie(0, order, 1), lie(1, order, -1), lie(1, order, 1)),
        arrived + swapped,
        q, wk, wv, state, False, scales,
    )
    low_swap = swap(far_low)
    high_swap = swap(far_high)
    attention = attend(
        info, (lie(0, order, 2), lie(1, order, 2)),
        [far_low, far_high, low_swap, high_swap],
        q, wk, wv, state, True, scales,
    )

    attention_other = swap(attention)
    low, wide = jnp.bfloat16, jnp.float32
    types = [wide, wide, wide, wide, wide, low, low, wide]
    project_args = (attention, attention_other, out_weight[0], out_other)
    body, specs, scratch = fetched(project_kernel, 1, project_args)
    a_m1, a_p1, a_m2, a_p2, a_m3, a_p3, a_m4, here = pl.pallas_call(
        body,
        in_specs=[SMEM] + specs,
        scratch_shapes=scratch,
        out_specs=[VMEM] * 8,
        out_shape=[jax.ShapeDtypeStruct((row_count, width), t) for t in types],
        cost_estimate=pl.CostEstimate(
            flops=2 * 192 * 512 * width, bytes_accessed=4 * 512 * width, transcendentals=0
        ),
        compiler_params=LARGE,
        name="project",
    )(info, *project_args)
    onward = ring(1)
    back = ring(-1)

    def hop(value, addend):
        return (send(value, back).astype(wide) + addend).astype(low)

    head_m = hop(a_m4, a_m3)
    head_p = hop(a_p3, a_p2)
    head_m = hop(head_m, a_m2)
    head_p = hop(head_p, a_p1)
    head_m = hop(head_m, a_m1)
    head_p = swap(send(head_p, back))
    head_m = send(head_m, back)
    head_total = here + head_m.astype(wide) + head_p.astype(wide)
    mixed_rows = residual.astype(jnp.float32) + head_total
    normed = rms_scale(mixed_rows, norm_gain).astype(jnp.bfloat16)

    experts_dev = gate_weight.shape[0]
    sp_count = NY * NX
    experts_all = experts_dev * sp_count
    top_count = routes.shape[1]
    slot_count = experts_all * CAP
    own_routes = lax.dynamic_slice_in_dim(routes, (iz * NC + core) * row_count, row_count, 0)
    own_slots = slot_table(own_routes, experts_all, CAP)
    pick_matrix = (
        jnp.arange(slot_count, dtype=jnp.int32)[:, None] == own_slots[None, :]
    ).astype(jnp.bfloat16)
    pick_matrix = pick_matrix.reshape(slot_count, row_count, top_count).sum(axis=2)
    outgoing = jnp.dot(pick_matrix, normed, preferred_element_type=jnp.float32).astype(jnp.bfloat16)
    arrived_rows = lax.all_to_all(
        outgoing.reshape(sp_count, experts_dev * CAP, width), SP, 0, 0, tiled=True
    ).reshape(slot_count, width)
    slot = jnp.arange(slot_count, dtype=jnp.int32)
    per = sp_count * CAP
    source = (slot % per) // CAP * (experts_dev * CAP) + slot // per * CAP + slot % CAP
    shuffle = (source[:, None] == slot[None, :]).astype(jnp.bfloat16)
    own = jnp.dot(shuffle, arrived_rows, preferred_element_type=jnp.float32).astype(jnp.bfloat16)

    block_bytes = slot_count * width * 2

    def hidden_of(mine, theirs):
        n = len(mine)
        shape = jax.ShapeDtypeStruct((experts_dev, n * per, gate_weight.shape[2]), jnp.bfloat16)
        keep, give = pl.pallas_call(
            functools.partial(hidden_kernel, n),
            in_specs=[VMEM] * (2 * n + 2),
            out_specs=[VMEM] * 2,
            out_shape=[shape] * 2,
            cost_estimate=pl.CostEstimate(
                flops=2 * 2 * n * slot_count * width * 512,
                bytes_accessed=2 * n * block_bytes + 4 * width * 512 * 2,
                transcendentals=2 * n * slot_count * 256,
            ),
            compiler_params=PARAMS,
            name="hidden",
        )(*mine, *theirs, gate_weight, up_weight)
        return keep, give

    down_shape = (experts_dev, 2 * down_weight.shape[1], width)
    down_both = pl.pallas_call(
        join_kernel,
        in_specs=[HBM, HBM],
        out_specs=VMEM,
        out_shape=jax.ShapeDtypeStruct(down_shape, jnp.bfloat16),
        scratch_shapes=[pltpu.SemaphoreType.DMA((2,))],
        cost_estimate=pl.CostEstimate(
            flops=1 << 22, bytes_accessed=1 << 23, transcendentals=0
        ),
        compiler_params=PARAMS,
        name="join",
    )(down_weight, down_other)

    def outputs_of(keep, got, types):
        result = [
            jnp.dot(
                jnp.concatenate([keep[e], got[e]], axis=1),
                down_both[e],
                preferred_element_type=wide,
            )
            for e in range(experts_dev)
        ]
        return [
            jnp.concatenate([r[i * per : (i + 1) * per] for r in result], axis=0).astype(t)
            for i, t in enumerate(types)
        ]

    m1 = send(own, onward)
    par = swap(own)
    p1 = send(par, onward)
    h0 = hidden_of([own], [par])
    m2 = send(m1, onward)
    sm1 = swap(m1)
    p2 = send(p1, onward)
    sp1 = swap(p1)
    h1 = hidden_of([m1, p1], [sm1, sp1])
    m3 = send(m2, onward)
    sm2 = swap(m2)
    p3 = send(p2, onward)
    sp2 = swap(p2)
    h2 = hidden_of([m2, p2], [sm2, sp2])
    m4 = send(m3, onward)
    sm3 = swap(m3)
    sp3 = swap(p3)
    h3 = hidden_of([m3, p3], [sm3, sp3])
    sm4 = swap(m4)
    h4 = hidden_of([m4], [sm4])
    o_m3, o_p3 = outputs_of(h3[0], swap(h3[1]), (wide, wide))
    (o_m4,) = outputs_of(h4[0], swap(h4[1]), (low,))
    keep, give = (jnp.concatenate(h, axis=1) for h in zip(h0, h1, h2))
    got = swap(give)
    o_own, o_m1, o_p1, o_m2, o_p2 = outputs_of(keep, got, (wide,) * 5)

    chain_p = hop(o_p3.astype(low), o_p2)
    chain_m = hop(o_m4, o_m3)
    chain_p = hop(chain_p, o_p1)
    chain_m = hop(chain_m, o_m2)
    chain_p = swap(send(chain_p, back))
    chain_m = hop(chain_m, o_m1)
    chain_m = send(chain_m, back)
    total = (o_own + chain_m.astype(wide) + chain_p.astype(wide)).astype(low)

    unshuffled = lax.dot_general(
        shuffle, total, (((0,), (0,)), ((), ())), preferred_element_type=jnp.float32
    ).astype(jnp.bfloat16)
    returned = lax.all_to_all(
        unshuffled.reshape(sp_count, experts_dev * CAP, width), SP, 0, 0, tiled=True
    ).reshape(slot_count, width)
    selectors = (own_slots[:, None] == slot[None, :]).astype(jnp.bfloat16)
    picked = jnp.dot(selectors, returned, preferred_element_type=jnp.float32).reshape(
        row_count, top_count, -1
    )
    route_weight = group_gate[:, None] * expert_share / jnp.sum(expert_share, axis=1, keepdims=True)
    expert_mix = jnp.sum(route_weight[:, :, None] * picked, axis=1)
    return (mixed_rows + expert_mix).astype(jnp.bfloat16)


def solution(mesh):
    finer = Mesh(mesh.devices.reshape(NY, NX, NZ, NC), AXES)
    tp = ("z", "c")
    placed = (
        P(AXES, None),
        P(SP, tp, None),
        P(SP, tp, None),
        P(SP, None),
        P(SP, None),
        P(),
        P(None, tp, None),
        P(None, tp, None),
        P(tp, None, None),
        P(),
        P(SP, None),
        P(AXES),
        P(AXES, None),
        P(SP, None, tp),
        P(SP, None, tp),
        P(SP, tp, None),
    )
    return jax.shard_map(
        layer, mesh=finer, in_specs=placed, out_specs=P(AXES, None), check_vma=False
    )
```
